256 devices in a mesh: fs: 16 (over y, x), tp: 16 (over z, core).
Axes of the slice: x: 4, y: 4, z: 8, core: 2. Of those that a mesh axis runs over, the one named last changes fastest.
Arguments:
- later_tokens: bfloat16 [14336, 2048], P(('fs', 'tp')), may hold values from -6 to 6
- earlier_tokens: bfloat16 [14336, 2048], P(('fs', 'tp')), may hold values from -6 to 6
- earlier_cotangent: bfloat16 [14336, 2048], P(('fs', 'tp')), may hold values from -24 to 24
- gate_weight: bfloat16 [2048, 5632], P('fs', 'tp'), may hold values from -0.125 to 0.125
- up_weight: bfloat16 [2048, 5632], P('fs', 'tp'), may hold values from -0.125 to 0.125
- down_weight: bfloat16 [5632, 2048], P('tp', 'fs'), may hold values from -0.078125 to 0.078125
- gate_sum: float32 [2048, 5632], P('fs', 'tp'), may hold values from -48 to 48
- up_sum: float32 [2048, 5632], P('fs', 'tp'), may hold values from -48 to 48
- down_sum: float32 [5632, 2048], P('tp', 'fs'), may hold values from -48 to 48
Outputs:
- later_output: bfloat16 [14336, 2048], P(('fs', 'tp'))
- earlier_grad: bfloat16 [14336, 2048], P(('fs', 'tp'))
- gate_total: float32 [2048, 5632], P('fs', 'tp')
- up_total: float32 [2048, 5632], P('fs', 'tp')
- down_total: float32 [5632, 2048], P('tp', 'fs')
The draws below stay inside these ranges and needn't reach their ends.
All inputs are finite; a program needn't handle non-finite values.
Results may differ from the reference program's by a relative error of at most 0.018.
Values may be sent and summed in bfloat16 or wider, within the bound.
No kernel may reach another device: no remote copies, remote signals or barrier semaphores. Data moves between devices by JAX's collectives and lax.ppermute only.
A program may use at most 128 MiB of HBM per device.

```python
import jax
import jax.numpy as jnp
from jax import lax

D = 2048
FF = 5632
TOKENS = 14336
N_TP = 16


def raised(entries, key, source, target, shards_of, factor):
    owner, partner = [(jnp.arange(entries.shape[dim]) // (entries.shape[dim] // shards_of)).reshape([-1 if axis == dim else 1 for axis in range(entries.ndim)]) for dim in (source, target)]
    chosen = jax.random.permutation(key, shards_of)[partner]
    strong = (owner == chosen) | (owner == (partner + shards_of // 2) % shards_of)
    return jnp.where(strong, factor * entries, entries)


def levels(own_key, extent, split, low, high):
    level, own = 1.0, jax.random.fold_in(own_key, 6)
    for dim, shards_of in split:
        steps = jnp.exp(jax.random.uniform(jax.random.fold_in(own, dim), (shards_of,), jnp.float32, low / len(split), high / len(split)))
        level = level * jnp.repeat(steps, extent[dim] // shards_of).reshape([-1 if axis == dim else 1 for axis in range(len(extent))])
    return level


def centred(rng, shape, deviation, limit, cuts=(), kind=jnp.bfloat16):
    values = deviation * jax.random.normal(rng, shape, jnp.float32)
    if cuts:
        values = values * levels(rng, shape, cuts, -0.22, 0.18)
    return jnp.clip(values, -limit, limit).astype(kind)


def heavy_noise(own_key, dims, spread, reach, shards, heavy, held_as=jnp.bfloat16):
    drawn = spread * jax.random.normal(own_key, dims, jnp.float32)
    if shards:
        drawn = drawn * levels(own_key, dims, shards, -0.22, 0.18)
    return jnp.clip(raised(drawn, jax.random.fold_in(own_key, 3), *heavy), -reach, reach).astype(held_as)


def setup_inputs(seed: int = 0) -> dict:
    key_of = jax.random.split(jax.random.key(seed), 10)
    return {
        "later_tokens": centred(key_of[0], (TOKENS, D), 1.0, 6.0, ((0, 256),)),
        "earlier_tokens": centred(key_of[1], (TOKENS, D), 1.0, 6.0, ((0, 256),)),
        "earlier_cotangent": heavy_noise(key_of[2], (TOKENS, D), 1.0, 24.0, ((0, 256),), (0, 1, 256, 6.0)),
        "gate_weight": centred(key_of[3], (D, FF), D ** -0.5, 0.125, ((0, 16), (1, 16))),
        "up_weight": centred(key_of[4], (D, FF), D ** -0.5, 0.125, ((0, 16), (1, 16))),
        "down_weight": centred(key_of[5], (FF, D), FF ** -0.5, 0.078125, ((0, 16), (1, 16))),
        "gate_sum": centred(key_of[6], (D, FF), 8.0, 48.0, ((0, 16), (1, 16)), jnp.float32),
        "up_sum": centred(key_of[7], (D, FF), 8.0, 48.0, ((0, 16), (1, 16)), jnp.float32),
        "down_sum": centred(key_of[8], (FF, D), 8.0, 48.0, ((0, 16), (1, 16)), jnp.float32),
    }


def blocked_sum(lefts, rights, rows):
    def step(total, pair):
        lhs, rhs = pair
        part = jnp.zeros((rows, D), jnp.float32)
        for left, right in zip(lhs, rhs):
            part = part + jnp.dot(left, right, preferred_element_type=jnp.float32)
        part = lax.optimization_barrier(part.astype(jnp.bfloat16))
        return total + part.astype(jnp.float32), None

    total, unused = lax.scan(step, jnp.zeros((rows, D), jnp.float32), (lefts, rights))
    return total.astype(jnp.bfloat16)


def split_columns(matrix):
    rows = matrix.shape[0]
    return matrix.reshape(rows, N_TP, FF // N_TP).transpose(1, 0, 2)


def split_rows(matrix):
    return matrix.reshape(N_TP, FF // N_TP, matrix.shape[1])


def reference(later_tokens, earlier_tokens, earlier_cotangent, gate_weight, up_weight, down_weight, gate_sum, up_sum, down_sum):
    rows = later_tokens.shape[0]
    later_gate = jnp.dot(later_tokens, gate_weight, preferred_element_type=jnp.float32)
    later_up = jnp.dot(later_tokens, up_weight, preferred_element_type=jnp.float32)
    later_hidden = (jax.nn.silu(later_gate) * later_up).astype(jnp.bfloat16)
    later_output = blocked_sum((split_columns(later_hidden),), (split_rows(down_weight),), rows)

    earlier_gate = jnp.dot(earlier_tokens, gate_weight, preferred_element_type=jnp.float32)
    earlier_up = jnp.dot(earlier_tokens, up_weight, preferred_element_type=jnp.float32)
    sigmoid_gate = jax.nn.sigmoid(earlier_gate)
    earlier_act = earlier_gate * sigmoid_gate
    earlier_hidden = (earlier_act * earlier_up).astype(jnp.bfloat16)
    hidden_grad = jnp.dot(earlier_cotangent, down_weight.T, preferred_element_type=jnp.float32)
    slope = sigmoid_gate * (1.0 + earlier_gate * (1.0 - sigmoid_gate))
    gate_grad = (hidden_grad * earlier_up * slope).astype(jnp.bfloat16)
    up_grad = (hidden_grad * earlier_act).astype(jnp.bfloat16)
    earlier_grad = blocked_sum((split_columns(gate_grad), split_columns(up_grad)),
                               (split_rows(gate_weight.T), split_rows(up_weight.T)), rows)

    gate_total = gate_sum + jnp.dot(earlier_tokens.T, gate_grad, preferred_element_type=jnp.float32)
    up_total = up_sum + jnp.dot(earlier_tokens.T, up_grad, preferred_element_type=jnp.float32)
    down_total = down_sum + jnp.dot(earlier_hidden.T, earlier_cotangent, preferred_element_type=jnp.float32)
    return later_output, earlier_grad, gate_total, up_total, down_total
```

```python
import functools

import jax
import jax.numpy as jnp
from jax import lax
from jax.experimental import pallas as pl
from jax.experimental.pallas import tpu as pltpu
from jax.sharding import Mesh
from jax.sharding import PartitionSpec as P

NY, NX, NZ = 4, 4, 8
LANES = 128
F32, BF16 = jnp.float32, jnp.bfloat16
VMEM = pl.BlockSpec(memory_space=pltpu.VMEM)
SMEM = pl.BlockSpec(memory_space=pltpu.SMEM)


def z_pairs(step):
    return [
        (z * 2 + c, (z + (step if c == 0 else -step)) % NZ * 2 + c)
        for z in range(NZ)
        for c in range(2)
    ]


def plane_pairs(step, stage):
    pairs = []
    for y in range(NY):
        for x in range(NX):
            for c in range(2):
                along_x = (stage == 1) == (c == 0)
                to_y = y if along_x else (y + step) % NY
                to_x = (x + step) % NX if along_x else x
                pairs.append(((y * NX + x) * 2 + c, (to_y * NX + to_x) * 2 + c))
    return pairs


def z_send(value, step):
    return lax.ppermute(value, ("z", "c"), z_pairs(step))


def plane_send(value, step, stage):
    return lax.ppermute(value, ("y", "x", "c"), plane_pairs(step, stage))


def swap(value):
    return lax.ppermute(value, "c", [(0, 1), (1, 0)])


def call(kernel, outs, ins, flops=0, scalars=0):
    moved = sum(o.size * o.dtype.itemsize for o in outs) + sum(i.size * i.dtype.itemsize for i in ins)
    return pl.pallas_call(
        kernel,
        out_shape=outs,
        in_specs=[SMEM] * scalars + [VMEM] * (len(ins) - scalars),
        out_specs=[VMEM] * len(outs),
        compiler_params=pltpu.CompilerParams(vmem_limit_bytes=40 * 2**20),
        cost_estimate=pl.CostEstimate(flops=flops or moved, bytes_accessed=moved, transcendentals=0),
    )(*ins)


def like(shape, dtype):
    return jax.ShapeDtypeStruct(shape, dtype)


def lane(k):
    return pl.ds(k * LANES, LANES)


def pack_weights_kernel(gate_ref, up_ref, down_ref, out_ref):
    rows = gate_ref.shape[0]
    for k, ref in enumerate((gate_ref, up_ref, down_ref)):
        out_ref[k * rows : (k + 1) * rows, :] = ref[...]


def pack_tokens_kernel(place_ref, *refs):
    ins, (earlier_ref, later_ref) = refs[:6], refs[6:]
    rows = ins[0].shape[0]
    blocks = ins[0].shape[1] // LANES
    for k in range(blocks):
        at = pl.ds(pl.multiple_of(place_ref[k] * LANES, LANES), LANES)
        for half in range(2):
            to = slice(half * rows, (half + 1) * rows)
            earlier_ref[to, lane(k)] = ins[half][:, at]
            earlier_ref[to, lane(blocks + k)] = ins[2 + half][:, at]
            later_ref[to, lane(k)] = ins[4 + half][:, at]


def unpack_kernel(own_place_ref, other_place_ref, kept_ref, mine_ref, other_ref, out_ref):
    rows = kept_ref.shape[0]
    for k in range(out_ref.shape[1] // LANES):
        own = pl.ds(pl.multiple_of(own_place_ref[k] * LANES, LANES), LANES)
        other = pl.ds(pl.multiple_of(other_place_ref[k] * LANES, LANES), LANES)
        total = kept_ref[:, own].astype(F32) + mine_ref[:, own].astype(F32) + other_ref[:, other].astype(F32)
        out_ref[:, lane(k)] = total.astype(BF16)


def assemble_kernel(*refs):
    own, other, outs = refs[:5], refs[5:10], refs[10:]
    hidden = own[0].shape[0] // 3

    def rows_of(pieces, b, k, a):
        if b != 2:
            ref = pieces[{0: 0, 1: 1, 3: 2}[b]]
            return [(0, hidden, ref, k * hidden)]
        half = own[3].shape[0]
        lo, hi = k * hidden, (k + 1) * hidden
        spans = []
        if lo < half:
            spans.append((0, min(hi, half) - lo, pieces[3], lo))
        if hi > half:
            start = max(lo, half)
            spans.append((start - lo, hi - start, pieces[4], start - half))
        return spans

    for k in range(3):
        for b in range(4):
            for a in range(4):
                for to, count, ref, at in rows_of(own, b, k, a):
                    outs[k][to : to + count, lane(b * 4 + a)] = ref[at : at + count, lane(a)]
                for to, count, ref, at in rows_of(other, b, k, a):
                    to = to + hidden
                    outs[k][to : to + count, lane(a * 4 + b)] = ref[at : at + count, lane(a)]


def pair_sum_kernel(*refs):
    own, other, outs = refs[:3], refs[3:6], refs[6:]
    rows = own[0].shape[0]
    for b in range(4):
        for a in range(4):
            for k in range(3):
                total = own[k][:, lane(b * 4 + a)] + other[k][:, lane(a * 4 + b)].astype(F32)
                outs[b][k * rows : (k + 1) * rows, lane(a)] = total.astype(outs[b].dtype)


def ring_gather(block, stage):
    half = block.shape[0] // 2
    before = plane_send(block, 1, stage)
    after = plane_send(block, -1, stage)
    far_top = plane_send(before[:half], 1, stage)
    far_bottom = plane_send(after[half:], -1, stage)
    return after, before, far_top, far_bottom


def ring_sum(here, after, far, before, stage):
    half = far.shape[0] // 2
    top = plane_send(far[:half].astype(BF16), 1, stage)
    bottom = plane_send(far[half:].astype(BF16), -1, stage)
    up = jnp.concatenate([after[:half] + top.astype(F32), after[half:]], axis=0).astype(BF16)
    down = jnp.concatenate([before[:half], before[half:] + bottom.astype(F32)], axis=0).astype(BF16)
    from_before = plane_send(up, 1, stage)
    from_after = plane_send(down, -1, stage)
    return here + from_before.astype(F32) + from_after.astype(F32)


def dot(left, right, left_dim, right_dim):
    return lax.dot_general(
        left, right, (((left_dim,), (right_dim,)), ((), ())), preferred_element_type=F32
    )


def z_gather(block):
    rows = block.shape[0] // 2
    one = z_send(block, 1)
    two = z_send(one, 1)
    three = z_send(two, 1)
    four = z_send(three[:rows], 1)
    return jnp.concatenate([one, two, three, block[:rows], four], axis=0)


def z_sum(terms):
    pair = terms.shape[0] // 4
    rows = pair // 2
    one, two, three = (terms[k * pair : (k + 1) * pair] for k in range(3))
    kept, four = terms[3 * pair : 3 * pair + rows], terms[3 * pair + rows :]
    got = z_send(four.astype(BF16), -1)
    three = jnp.concatenate([three[:rows] + got.astype(F32), three[rows:]], axis=0)
    got = z_send(three.astype(BF16), -1)
    got = z_send((two + got.astype(F32)).astype(BF16), -1)
    got = z_send((one + got.astype(F32)).astype(BF16), -1)
    return kept, got[:rows], swap(got[rows:])


def body(later_tokens, earlier_tokens, earlier_cotangent, gate_weight, up_weight, down_weight, gate_sum, up_sum, down_sum):
    tokens, width = later_tokens.shape
    hidden = down_weight.shape[0]
    y, x, c = lax.axis_index("y"), lax.axis_index("x"), lax.axis_index("c")
    k = jnp.arange(16, dtype=jnp.int32)
    high, low = k // 4, k % 4
    order0 = (y + high) % NY * NX + (x + low) % NX
    order1 = (y + low) % NY * NX + (x + high) % NX
    place0 = (high - y) % NY * 4 + (low - x) % NX
    place1 = (low - x) % NX * 4 + (high - y) % NY
    order = jnp.where(c == 0, order0, order1)
    own_place = jnp.where(c == 0, place0, place1)
    other_place = jnp.where(c == 0, place1, place0)

    packed = call(pack_weights_kernel, [like((3 * hidden, LANES), BF16)], [gate_weight.T, up_weight.T, down_weight])[0]
    after, before, far_top, far_bottom = ring_gather(packed, 1)
    line = jnp.concatenate([packed, after, jnp.concatenate([far_top, far_bottom], axis=0), before], axis=1)
    after, before, far_top, far_bottom = ring_gather(line, 2)
    pieces = [line, after, before, far_top, far_bottom]
    others = [swap(p) for p in pieces]
    full = like((2 * hidden, width), BF16)
    gate_w, up_w, down_w = call(assemble_kernel, [full] * 3, pieces + others)

    ins = []
    for a in (earlier_tokens, earlier_cotangent, later_tokens):
        ins += [a, swap(a)]
    earlier_block, later_block = call(
        pack_tokens_kernel,
        [like((2 * tokens, 2 * width), BF16), like((2 * tokens, width), BF16)],
        [order] + ins,
        scalars=1,
    )
    earlier = z_gather(earlier_block)
    later = z_gather(later_block)
    group_tokens, group_cotangent = earlier[:, :width], earlier[:, width:]

    earlier_gate = dot(group_tokens, gate_w, 1, 1)
    earlier_up = dot(group_tokens, up_w, 1, 1)
    hidden_grad = dot(group_cotangent, down_w, 1, 1)
    sigmoid_gate = jax.nn.sigmoid(earlier_gate)
    earlier_act = earlier_gate * sigmoid_gate
    earlier_hidden = (earlier_act * earlier_up).astype(BF16)
    slope = sigmoid_gate * (1.0 + earlier_gate * (1.0 - sigmoid_gate))
    gate_grad = (hidden_grad * earlier_up * slope).astype(BF16)
    up_grad = (hidden_grad * earlier_act).astype(BF16)

    terms = dot(gate_grad, gate_w, 1, 0) + dot(up_grad, up_w, 1, 0)
    kept, mine, other = z_sum(terms)
    earlier_grad = call(unpack_kernel, [like((tokens, width), BF16)], [own_place, other_place, kept, mine, other], scalars=2)[0]

    parts = ((gate_grad, group_tokens), (up_grad, group_tokens), (earlier_hidden, group_cotangent))
    sent = [swap(dot(left[:, hidden:], right, 0, 0).astype(BF16)) for left, right in parts]
    held = [dot(left[:, :hidden], right, 0, 0) for left, right in parts]
    piece = like((3 * hidden, width // 4), F32)
    four = call(pair_sum_kernel, [piece] * 4, held + sent)
    line = ring_sum(*four, 2)
    total = ring_sum(*(line[:, k * LANES : (k + 1) * LANES] for k in range(4)), 1)
    gate_total = gate_sum + total[:hidden].T
    up_total = up_sum + total[hidden : 2 * hidden].T
    down_total = down_sum + total[2 * hidden :]

    later_gate = dot(later, gate_w, 1, 1)
    later_up = dot(later, up_w, 1, 1)
    later_hidden = (jax.nn.silu(later_gate) * later_up).astype(BF16)
    terms = dot(later_hidden, down_w, 1, 0)
    kept, mine, other = z_sum(terms)
    later_output = call(unpack_kernel, [like((tokens, width), BF16)], [own_place, other_place, kept, mine, other], scalars=2)[0]
    return later_output, earlier_grad, gate_total, up_total, down_total


def solution(mesh):
    finer = Mesh(mesh.devices.reshape(NY, NX, NZ, 2), ("y", "x", "z", "c"))
    rows, cols = ("y", "x"), ("z", "c")
    token = P(rows + cols, None)
    in_specs = (token,) * 3 + (P(rows, cols), P(rows, cols), P(cols, rows)) * 2
    out_specs = (token, token, P(rows, cols), P(rows, cols), P(cols, rows))
    return jax.shard_map(body, mesh=finer, in_specs=in_specs, out_specs=out_specs, check_vma=False)
```

```python
import functools

import jax
import jax.numpy as jnp
from jax import lax
from jax.experimental import pallas as pl
from jax.experimental.pallas import tpu as pltpu
from jax.sharding import Mesh
from jax.sharding import PartitionSpec as P


NY, NX, NZ = 4, 4, 8
LANES = 128
TILE = 1024
STEP = 16
F32, BF16 = jnp.float32, jnp.bfloat16
VMEM = pl.BlockSpec(memory_space=pltpu.VMEM)
SMEM = pl.BlockSpec(memory_space=pltpu.SMEM)


def z_pairs(step):
    return [
        (z * 2 + c, (z + (step if c == 0 else -step)) % NZ * 2 + c)
        for z in range(NZ)
        for c in range(2)
    ]


def plane_pairs(step, stage):
    pairs = []
    for y in range(NY):
        for x in range(NX):
            for c in range(2):
                along_x = (stage == 1) == (c == 0)
                to_y = y if along_x else (y + step) % NY
                to_x = (x + step) % NX if along_x else x
                pairs.append(((y * NX + x) * 2 + c, (to_y * NX + to_x) * 2 + c))
    return pairs


def z_send(value, step):
    return lax.ppermute(value, ("z", "c"), z_pairs(step))


def plane_send(value, step, stage):
    return lax.ppermute(value, ("y", "x", "c"), plane_pairs(step, stage))


def swap(value):
    return lax.ppermute(value, "c", [(0, 1), (1, 0)])


def call(kernel, outs, ins, specs=None, flops=0, scratch=(), limit=4):
    moved = sum(o.size * o.dtype.itemsize for o in outs) + sum(i.size * i.dtype.itemsize for i in ins)
    return pl.pallas_call(
        kernel,
        out_shape=outs,
        in_specs=specs or [VMEM] * len(ins),
        out_specs=[VMEM] * len(outs),
        scratch_shapes=scratch,
        compiler_params=pltpu.CompilerParams(vmem_limit_bytes=int(limit * 2**20)),
        cost_estimate=pl.CostEstimate(flops=flops or moved, bytes_accessed=moved, transcendentals=0),
    )(*ins)


def like(shape, dtype):
    return jax.ShapeDtypeStruct(shape, dtype)


def lane(k):
    return pl.ds(k * LANES, LANES)


def pack_tokens_kernel(place_ref, own_ref, other_ref, earlier_ref, later_ref):
    rows, width = own_ref.shape[0], later_ref.shape[1]
    blocks = width // LANES
    for k in range(blocks):
        start = place_ref[k] * LANES
        for half, ref in enumerate((own_ref, other_ref)):
            to = slice(half * rows, (half + 1) * rows)
            for n, (out, first) in enumerate(((earlier_ref, 0), (earlier_ref, blocks), (later_ref, 0))):
                out[to, lane(first + k)] = ref[:, pl.ds(pl.multiple_of(n * width + start, LANES), LANES)]


def last_add_kernel(earlier_ref, later_ref, earlier_got, later_got, out_ref):
    rows, width = earlier_got.shape
    for n, (ref, got) in enumerate(((earlier_ref, earlier_got), (later_ref, later_got))):
        out_ref[:, n * width : (n + 1) * width] = (ref[:rows, :] + got[...].astype(F32)).astype(BF16)


def unpack_kernel(own_place_ref, other_place_ref, *refs):
    kept, mine_ref, other_ref, outs = refs[:2], refs[2], refs[3], refs[4:]
    width = kept[0].shape[1]
    rows = other_ref.shape[0]
    for k in range(width // LANES):
        own = pl.multiple_of(own_place_ref[k] * LANES, LANES)
        other = pl.multiple_of(other_place_ref[k] * LANES, LANES)
        for n in range(2):
            total = (
                kept[n][kept[n].shape[0] - 2 * rows : kept[n].shape[0] - rows, pl.ds(own, LANES)]
                + mine_ref[:rows, pl.ds(n * width + own, LANES)].astype(F32)
                + other_ref[:, pl.ds(n * width + other, LANES)].astype(F32)
            )
            outs[n][:, lane(k)] = total.astype(BF16)


def z_add_kernel(first, terms_ref, *refs):
    got, out = refs[0] if len(refs) > 1 else None, refs[-1]
    rows = out.shape[0]
    more = got.shape[0] if got is not None else 0
    if more:
        out[:more, :] = (terms_ref[first : first + more, :] + got[...].astype(F32)).astype(BF16)
    if more < rows:
        out[more:, :] = terms_ref[first + more : first + rows, :].astype(BF16)


def line_sum_kernel(here, from_before, from_after, *outs):
    rows = here.shape[0]

    @pl.loop(0, rows // STEP)
    def _(i):
        at = pl.ds(pl.multiple_of(i * STEP, STEP), STEP)
        for k, out in enumerate(outs):
            total = here[at, lane(k)] + from_before[at, lane(k)].astype(F32) + from_after[at, lane(k)].astype(F32)
            out[at, :] = total.astype(out.dtype)


def add_kernel(left, right, out):
    @pl.loop(0, out.shape[0] // STEP)
    def _(i):
        at = pl.ds(pl.multiple_of(i * STEP, STEP), STEP)
        out[at, :] = (left[at, :] + right[at, :].astype(F32)).astype(out.dtype)


def assemble_kernel(*refs):
    pieces, out = (refs[:4], refs[4:8]), refs[8]
    hidden = pieces[0][0].shape[0] // 3

    @pl.loop(0, hidden // STEP)
    def _(i):
        row = pl.multiple_of(i * STEP, STEP)
        for k in range(3):
            for n, b in enumerate((0, 1, 3, 2)):
                for core in range(2):
                    for a in range(4):
                        place = a * 4 + b if core else b * 4 + a
                        strip = pieces[core][n][pl.ds(k * hidden + row, STEP), lane(a)]
                        out[k, pl.ds(core * hidden + row, STEP), lane(place)] = strip


def pair_sum_kernel(*refs):
    own, other, outs = refs[0], refs[1], refs[2:]
    rows = own.shape[1]

    @pl.loop(0, rows // STEP)
    def _(i):
        row = pl.multiple_of(i * STEP, STEP)
        for b in range(4):
            for a in range(4):
                for k in range(3):
                    at = pl.ds(k * rows + row, STEP)
                    total = own[k, pl.ds(row, STEP), lane(b * 4 + a)] + other[at, lane(a * 4 + b)].astype(F32)
                    outs[b][at, lane(a)] = total


def ring_add_kernel(after, before, top, bottom, up, down):
    half = top.shape[0]

    @pl.loop(0, half // STEP)
    def _(i):
        at = pl.ds(pl.multiple_of(i * STEP, STEP), STEP)
        low = pl.ds(pl.multiple_of(half + i * STEP, STEP), STEP)
        up[at, :] = (after[at, :] + top[at, :].astype(F32)).astype(BF16)
        up[low, :] = after[low, :].astype(BF16)
        down[at, :] = before[at, :].astype(BF16)
        down[low, :] = (before[low, :] + bottom[at, :].astype(F32)).astype(BF16)


def nt_dot(left, right):
    return lax.dot_general(left, right, (((1,), (1,)), ((), ())), preferred_element_type=F32)


def tn_dot(left, right):
    return lax.dot_general(left, right, (((0,), (0,)), ((), ())), preferred_element_type=F32)


def gather_rows(pieces, x_ref):
    at = 0
    for ref, rows in pieces:
        x_ref[at : at + rows, :] = ref[:rows, :]
        at += rows


def grads_kernel(counts, *refs):
    pieces, refs = refs[: len(counts)], refs[len(counts) :]
    weights, x_ref, grads, made = refs
    gather_rows(list(zip(pieces, counts)), x_ref)
    width = weights.shape[2]

    @pl.loop(0, 3)
    def _(k):
        first = pl.multiple_of(k // 2 * width, width)
        made[k] = nt_dot(x_ref[:, pl.ds(first, width)], weights[k])

    @pl.loop(0, x_ref.shape[0] // STEP)
    def _(i):
        rows = pl.ds(pl.multiple_of(i * STEP, STEP), STEP)
        g, u, h = made[0, rows, :], made[1, rows, :], made[2, rows, :]
        s = jax.nn.sigmoid(g)
        a = g * s
        grads[0, rows, :] = (h * u * (s * (1.0 + g * (1.0 - s)))).astype(BF16)
        grads[1, rows, :] = (h * a).astype(BF16)
        grads[2, rows, :] = (a * u).astype(BF16)


def terms_kernel(near, far, weights, terms, lefts):
    rows = near.shape[1]
    for k in range(2):
        lefts[k, :rows] = near[k]
        lefts[k, rows:] = far[k]

    @pl.loop(0, terms.shape[1] // TILE)
    def _(n):
        at = pl.ds(pl.multiple_of(n * TILE, TILE), TILE)
        terms[:, at] = jnp.dot(lefts[0], weights[0, :, at], preferred_element_type=F32) + jnp.dot(
            lefts[1], weights[1, :, at], preferred_element_type=F32
        )


def later_kernel(counts, *refs):
    pieces, refs = refs[: len(counts)], refs[len(counts) :]
    weights, terms, x_ref, made, act = refs
    gather_rows(list(zip(pieces, counts)), x_ref)

    @pl.loop(0, 2)
    def _(k):
        made[k] = nt_dot(x_ref[...], weights[k])

    @pl.loop(0, x_ref.shape[0] // STEP)
    def _(i):
        rows = pl.ds(pl.multiple_of(i * STEP, STEP), STEP)
        g = made[0, rows, :]
        act[rows, :] = (g * jax.nn.sigmoid(g) * made[1, rows, :]).astype(BF16)

    @pl.loop(0, terms.shape[1] // TILE)
    def _(n):
        at = pl.ds(pl.multiple_of(n * TILE, TILE), TILE)
        terms[:, at] = jnp.dot(act[...], weights[2, :, at], preferred_element_type=F32)


def weight_grads_kernel(grads, x_ref, here, there):
    rows, width = here.shape[1:]

    @pl.loop(0, 3)
    def _(k):
        @pl.loop(0, width // TILE)
        def _(n):
            to = pl.ds(pl.multiple_of(n * TILE, TILE), TILE)
            at = pl.ds(pl.multiple_of(k // 2 * width + n * TILE, TILE), TILE)
            total = tn_dot(grads[k], x_ref[:, at])
            here[k, :, to] = total[:rows]
            there[k, :, to] = total[rows:]


def more_weight_grads_kernel(grads, x_ref, here, there, sent, held):
    rows, width = held.shape[1:]

    @pl.loop(0, 3)
    def _(k):
        @pl.loop(0, width // TILE)
        def _(n):
            to = pl.ds(pl.multiple_of(n * TILE, TILE), TILE)
            at = pl.ds(pl.multiple_of(k // 2 * width + n * TILE, TILE), TILE)
            total = tn_dot(grads[k], x_ref[:, at])
            held[k, :, to] = here[k, :, to] + total[:rows]
            sent[pl.ds(pl.multiple_of(k * rows, STEP), rows), to] = (there[k, :, to] + total[rows:]).astype(BF16)


def ring_gather(block, stage):
    half = block.shape[0] // 2
    before_top = plane_send(block[:half], 1, stage)
    after_bottom = plane_send(block[half:], -1, stage)
    before_bottom = plane_send(block[half:], 1, stage)
    after_top = plane_send(block[:half], -1, stage)
    far_top = plane_send(before_top, 1, stage)
    far_bottom = plane_send(after_bottom, -1, stage)
    halves = ((after_top, after_bottom), (far_top, far_bottom), (before_top, before_bottom))
    return [block] + [jnp.concatenate(h, axis=0) for h in halves]


def short_ring_gather(block, stage):
    before = plane_send(block, 1, stage)
    after = plane_send(block, -1, stage)
    far = plane_send(before, 1, stage)
    return [block, after, far, before]


def ring_sum(after, far, before, stage):
    half = far.shape[0] // 2
    top = plane_send(far[:half].astype(BF16), 1, stage)
    bottom = plane_send(far[half:].astype(BF16), -1, stage)
    out = like(after.shape, BF16)
    up, down = call(ring_add_kernel, [out] * 2, [after, before, top, bottom])
    return plane_send(up, 1, stage), plane_send(down, -1, stage)


def short_ring_sum(after, far, before, stage):
    got = plane_send(far, 1, stage)
    from_after = plane_send(before, -1, stage)
    up = call(add_kernel, [like(after.shape, BF16)], [after, got])[0]
    return plane_send(up, 1, stage), from_after


def z_gather(block):
    rows = block.shape[0] // 2
    one = z_send(block, 1)
    two = z_send(one, 1)
    three = z_send(two, 1)
    four = z_send(three[:rows], 1)
    return (one, two), (three, block, four), (2 * rows, 2 * rows), (2 * rows, rows, rows)


def z_sum(parts):
    got = []
    for terms, first, count in reversed(parts):
        block = call(functools.partial(z_add_kernel, first), [like((count, terms.shape[1]), BF16)], [terms] + got)[0]
        got = [z_send(block, -1)]
    return got[0]


def body(later_tokens, earlier_tokens, earlier_cotangent, gate_weight, up_weight, down_weight, gate_sum, up_sum, down_sum):
    tokens, width = later_tokens.shape
    hidden = down_weight.shape[0]
    y, x, c = lax.axis_index("y"), lax.axis_index("x"), lax.axis_index("c")
    k = jnp.arange(16, dtype=jnp.int32)
    high, low = k // 4, k % 4
    order0 = (y + high) % NY * NX + (x + low) % NX
    order1 = (y + low) % NY * NX + (x + high) % NX
    place0 = (high - y) % NY * 4 + (low - x) % NX
    place1 = (low - x) % NX * 4 + (high - y) % NY
    order = jnp.where(c == 0, order0, order1)
    own_place = jnp.where(c == 0, place0, place1)
    other_place = jnp.where(c == 0, place1, place0)

    packed = jnp.concatenate([gate_weight.T, up_weight.T, down_weight], axis=0)
    line = jnp.concatenate(short_ring_gather(packed, 1), axis=1)
    line, after, far, before = ring_gather(line, 2)
    pieces = [line, after, before, far]
    others = [swap(p) for p in pieces]
    weights = call(assemble_kernel, [like((3, 2 * hidden, width), BF16)], pieces + others)

    own = jnp.concatenate([earlier_tokens, earlier_cotangent, later_tokens], axis=1)
    earlier_block, later_block = call(
        pack_tokens_kernel,
        [like((2 * tokens, 2 * width), BF16), like((2 * tokens, width), BF16)],
        [order, own, swap(own)],
        [SMEM] + [VMEM] * 2,
    )
    near, far, near_counts, far_counts = z_gather(earlier_block)
    later_near, later_far, _, _ = z_gather(later_block)
    rows = 4 * tokens
    units = 2 * hidden

    def earlier(pieces, counts):
        return call(
            functools.partial(grads_kernel, counts),
            [like((rows, 2 * width), BF16), like((3, rows, units), BF16)],
            list(pieces) + list(weights),
            flops=6 * rows * units * width,
            scratch=[pltpu.VMEM((3, rows, units), F32)],
            limit=6,
        )

    def later(pieces, counts):
        return call(
            functools.partial(later_kernel, counts),
            [like((rows, width), F32)],
            list(pieces) + list(weights),
            flops=6 * rows * units * width,
            scratch=[pltpu.VMEM((rows, width), BF16)]
            + [pltpu.VMEM((2, rows, units), F32), pltpu.VMEM((rows, units), BF16)],
            limit=6,
        )[0]

    x_a, grads_a = earlier(near, near_counts)
    x_b, grads_b = earlier(far, far_counts)
    terms = call(
        terms_kernel,
        [like((2 * rows, width), F32)],
        [grads_a, grads_b, *weights],
        flops=8 * rows * units * width,
        scratch=[pltpu.VMEM((2, 2 * rows, units), BF16)],
        limit=6,
    )[0]
    later_a = later(later_near, near_counts)
    later_b = later(later_far, far_counts)
    pair = 2 * tokens
    sums = [
        z_sum([(terms, pair, pair), (terms, 2 * pair, pair), (terms, 3 * pair + tokens, tokens)]),
        z_sum([(later_a, pair, pair), (later_b, 0, pair), (later_b, pair + tokens, tokens)]),
    ]
    both = call(last_add_kernel, [like((pair, 2 * width), BF16)], [terms, later_a] + sums)[0]
    mine = z_send(both, -1)
    other = swap(mine[tokens:])
    earlier_grad, later_output = call(
        unpack_kernel,
        [like((tokens, width), BF16)] * 2,
        [own_place, other_place, terms, later_b, mine, other],
        [SMEM] * 2 + [VMEM] * 4,
    )

    so_far = call(
        weight_grads_kernel,
        [like((3, hidden, width), F32)] * 2,
        [grads_a, x_a],
        flops=6 * rows * units * width,
        limit=6,
    )
    sent, held = call(
        more_weight_grads_kernel,
        [like((3 * hidden, width), BF16), like((3, hidden, width), F32)],
        [grads_b, x_b, *so_far],
        flops=6 * rows * units * width,
        limit=6,
    )
    sent = swap(sent)
    piece = like((3 * hidden, width // 4), F32)
    here, after, far, before = call(pair_sum_kernel, [piece] * 4, [held, sent])
    from_before, from_after = ring_sum(after, far, before, 2)
    strip = like((3 * hidden, LANES), F32)
    strip_sent = like((3 * hidden, LANES), BF16)
    here, after, far, before = call(
        line_sum_kernel, [strip, strip, strip_sent, strip_sent], [here, from_before, from_after]
    )
    from_before, from_after = short_ring_sum(after, far, before, 1)
    total = here + from_before.astype(F32) + from_after.astype(F32)
    gate_total = gate_sum + total[:hidden].T
    up_total = up_sum + total[hidden : 2 * hidden].T
    down_total = down_sum + total[2 * hidden :]
    return later_output, earlier_grad, gate_total, up_total, down_total


def solution(mesh):
    finer = Mesh(mesh.devices.reshape(NY, NX, NZ, 2), ("y", "x", "z", "c"))
    rows, cols = ("y", "x"), ("z", "c")
    token = P(rows + cols, None)
    in_specs = (token,) * 3 + (P(rows, cols), P(rows, cols), P(cols, rows)) * 2
    out_specs = (token, token, P(rows, cols), P(rows, cols), P(cols, rows))

    return jax.shard_map(body, mesh=finer, in_specs=in_specs, out_specs=out_specs, check_vma=False)
```

```python
import functools

import jax
import jax.numpy as jnp
from jax import lax
from jax.experimental import pallas as pl
from jax.experimental.pallas import tpu as pltpu
from jax.sharding import Mesh
from jax.sharding import PartitionSpec as P


NY, NX, NZ = 4, 4, 8
LANES = 128
TILE = 1024
STEP = 16
F32, BF16 = jnp.float32, jnp.bfloat16
VMEM = pl.BlockSpec(memory_space=pltpu.VMEM)
SMEM = pl.BlockSpec(memory_space=pltpu.SMEM)


def z_pairs(step):
    return [
        (z * 2 + c, (z + (step if c == 0 else -step)) % NZ * 2 + c)
        for z in range(NZ)
        for c in range(2)
    ]


def plane_pairs(step, stage):
    pairs = []
    for y in range(NY):
        for x in range(NX):
            for c in range(2):
                along_x = (stage == 1) == (c == 0)
                to_y = y if along_x else (y + step) % NY
                to_x = (x + step) % NX if along_x else x
                pairs.append(((y * NX + x) * 2 + c, (to_y * NX + to_x) * 2 + c))
    return pairs


def z_send(value, step):
    return lax.ppermute(value, ("z", "c"), z_pairs(step))


def plane_send(value, step, stage):
    return lax.ppermute(value, ("y", "x", "c"), plane_pairs(step, stage))


def swap(value):
    return lax.ppermute(value, "c", [(0, 1), (1, 0)])


def call(kernel, outs, ins, specs=None, flops=0, scratch=(), limit=4):
    moved = sum(o.size * o.dtype.itemsize for o in outs) + sum(i.size * i.dtype.itemsize for i in ins)
    return pl.pallas_call(
        kernel,
        out_shape=outs,
        in_specs=specs or [VMEM] * len(ins),
        out_specs=[VMEM] * len(outs),
        scratch_shapes=scratch,
        compiler_params=pltpu.CompilerParams(vmem_limit_bytes=int(limit * 2**20)),
        cost_estimate=pl.CostEstimate(flops=flops or moved, bytes_accessed=moved, transcendentals=0),
    )(*ins)


def like(shape, dtype):
    return jax.ShapeDtypeStruct(shape, dtype)


def lane(k):
    return pl.ds(k * LANES, LANES)


def pack_tokens_kernel(place_ref, own_ref, other_ref, earlier_ref, later_ref):
    rows, width = own_ref.shape[0], later_ref.shape[1]
    blocks = width // LANES
    for k in range(blocks):
        start = place_ref[k] * LANES
        for half, ref in enumerate((own_ref, other_ref)):
            to = slice(half * rows, (half + 1) * rows)
            for n, (out, first) in enumerate(((earlier_ref, 0), (earlier_ref, blocks), (later_ref, 0))):
                out[to, lane(first + k)] = ref[:, pl.ds(pl.multiple_of(n * width + start, LANES), LANES)]


def last_add_kernel(earlier_ref, later_ref, earlier_got, later_got, out_ref):
    rows, width = earlier_got.shape
    for n, (ref, got) in enumerate(((earlier_ref, earlier_got), (later_ref, later_got))):
        out_ref[:, n * width : (n + 1) * width] = (ref[:rows, :] + got[...].astype(F32)).astype(BF16)


def unpack_kernel(own_place_ref, other_place_ref, *refs):
    kept, mine_ref, other_ref, outs = refs[:2], refs[2], refs[3], refs[4:]
    width = kept[0].shape[1]
    rows = other_ref.shape[0]
    for k in range(width // LANES):
        own = pl.multiple_of(own_place_ref[k] * LANES, LANES)
        other = pl.multiple_of(other_place_ref[k] * LANES, LANES)
        for n in range(2):
            total = (
                kept[n][kept[n].shape[0] - 2 * rows : kept[n].shape[0] - rows, pl.ds(own, LANES)]
                + mine_ref[:rows, pl.ds(n * width + own, LANES)].astype(F32)
                + other_ref[:, pl.ds(n * width + other, LANES)].astype(F32)
            )
            outs[n][:, lane(k)] = total.astype(BF16)


def z_add_kernel(first, terms_ref, *refs):
    got, out = refs[0] if len(refs) > 1 else None, refs[-1]
    rows = out.shape[0]
    more = got.shape[0] if got is not None else 0
    if more:
        out[:more, :] = (terms_ref[first : first + more, :] + got[...].astype(F32)).astype(BF16)
    if more < rows:
        out[more:, :] = terms_ref[first + more : first + rows, :].astype(BF16)


def line_sum_kernel(here, from_before, from_after, *outs):
    rows = here.shape[0]

    @pl.loop(0, rows // STEP)
    def _(i):
        at = pl.ds(pl.multiple_of(i * STEP, STEP), STEP)
        for k, out in enumerate(outs):
            total = here[at, lane(k)] + from_before[at, lane(k)].astype(F32) + from_after[at, lane(k)].astype(F32)
            out[at, :] = total.astype(out.dtype)


def assemble_kernel(*refs):
    pieces, out = (refs[:4], refs[4:8]), refs[8]
    hidden = pieces[0][0].shape[0] // 3

    @pl.loop(0, hidden // STEP)
    def _(i):
        row = pl.multiple_of(i * STEP, STEP)
        for k in range(3):
            for n, b in enumerate((0, 1, 3, 2)):
                for core in range(2):
                    for a in range(4):
                        place = a * 4 + b if core else b * 4 + a
                        strip = pieces[core][n][pl.ds(k * hidden + row, STEP), lane(a)]
                        out[k, pl.ds(core * hidden + row, STEP), lane(place)] = strip


def pair_sum_kernel(*refs):
    own, other, outs = refs[0], refs[1], refs[2:]
    rows = own.shape[1]

    @pl.loop(0, rows // STEP)
    def _(i):
        row = pl.multiple_of(i * STEP, STEP)
        for b in range(4):
            for a in range(4):
                for k in range(3):
                    at = pl.ds(k * rows + row, STEP)
                    total = own[k, pl.ds(row, STEP), lane(b * 4 + a)] + other[at, lane(a * 4 + b)].astype(F32)
                    outs[b][at, lane(a)] = total


def ring_add_kernel(after, before, top, bottom, up, down):
    half = top.shape[0]

    @pl.loop(0, half // STEP)
    def _(i):
        at = pl.ds(pl.multiple_of(i * STEP, STEP), STEP)
        low = pl.ds(pl.multiple_of(half + i * STEP, STEP), STEP)
        up[at, :] = (after[at, :] + top[at, :].astype(F32)).astype(BF16)
        up[low, :] = after[low, :].astype(BF16)
        down[at, :] = before[at, :].astype(BF16)
        down[low, :] = (before[low, :] + bottom[at, :].astype(F32)).astype(BF16)


def nt_dot(left, right):
    return lax.dot_general(left, right, (((1,), (1,)), ((), ())), preferred_element_type=F32)


def tn_dot(left, right):
    return lax.dot_general(left, right, (((0,), (0,)), ((), ())), preferred_element_type=F32)


def gather_rows(pieces, x_ref):
    at = 0
    for ref, rows in pieces:
        x_ref[at : at + rows, :] = ref[:rows, :]
        at += rows


def grads_kernel(counts, *refs):
    pieces, refs = refs[: len(counts)], refs[len(counts) :]
    weights, x_ref, grads, made = refs
    gather_rows(list(zip(pieces, counts)), x_ref)
    width = weights.shape[2]

    @pl.loop(0, 3)
    def _(k):
        first = pl.multiple_of(k // 2 * width, width)
        made[k] = nt_dot(x_ref[:, pl.ds(first, width)], weights[k])

    @pl.loop(0, x_ref.shape[0] // STEP)
    def _(i):
        rows = pl.ds(pl.multiple_of(i * STEP, STEP), STEP)
        g, u, h = made[0, rows, :], made[1, rows, :], made[2, rows, :]
        s = jax.nn.sigmoid(g)
        a = g * s
        grads[0, rows, :] = (h * u * (s * (1.0 + g * (1.0 - s)))).astype(BF16)
        grads[1, rows, :] = (h * a).astype(BF16)
        grads[2, rows, :] = (a * u).astype(BF16)


def terms_kernel(near, far, weights, terms, lefts):
    rows = near.shape[1]
    for k in range(2):
        lefts[k, :rows] = near[k]
        lefts[k, rows:] = far[k]

    @pl.loop(0, terms.shape[1] // TILE)
    def _(n):
        at = pl.ds(pl.multiple_of(n * TILE, TILE), TILE)
        terms[:, at] = jnp.dot(lefts[0], weights[0, :, at], preferred_element_type=F32) + jnp.dot(
            lefts[1], weights[1, :, at], preferred_element_type=F32
        )


def later_kernel(counts, *refs):
    pieces, refs = refs[: len(counts)], refs[len(counts) :]
    weights, terms, x_ref, made, act = refs
    gather_rows(list(zip(pieces, counts)), x_ref)

    @pl.loop(0, 2)
    def _(k):
        made[k] = nt_dot(x_ref[...], weights[k])

    @pl.loop(0, x_ref.shape[0] // STEP)
    def _(i):
        rows = pl.ds(pl.multiple_of(i * STEP, STEP), STEP)
        g = made[0, rows, :]
        act[rows, :] = (g * jax.nn.sigmoid(g) * made[1, rows, :]).astype(BF16)

    @pl.loop(0, terms.shape[1] // TILE)
    def _(n):
        at = pl.ds(pl.multiple_of(n * TILE, TILE), TILE)
        terms[:, at] = jnp.dot(act[...], weights[2, :, at], preferred_element_type=F32)


def weight_grads_kernel(grads, x_ref, here, there):
    rows, width = here.shape[1:]

    @pl.loop(0, 3)
    def _(k):
        @pl.loop(0, width // TILE)
        def _(n):
            to = pl.ds(pl.multiple_of(n * TILE, TILE), TILE)
            at = pl.ds(pl.multiple_of(k // 2 * width + n * TILE, TILE), TILE)
            total = tn_dot(grads[k], x_ref[:, at])
            here[k, :, to] = total[:rows]
            there[k, :, to] = total[rows:].astype(BF16)


def more_weight_grads_kernel(grads, x_ref, here, there, sent, held):
    rows, width = held.shape[1:]

    @pl.loop(0, 3)
    def _(k):
        @pl.loop(0, width // TILE)
        def _(n):
            to = pl.ds(pl.multiple_of(n * TILE, TILE), TILE)
            at = pl.ds(pl.multiple_of(k // 2 * width + n * TILE, TILE), TILE)
            total = tn_dot(grads[k], x_ref[:, at])
            held[k, :, to] = here[k, :, to] + total[:rows]
            sent[pl.ds(pl.multiple_of(k * rows, STEP), rows), to] = (there[k, :, to].astype(F32) + total[rows:]).astype(BF16)


def join_kernel(*refs):
    outs = refs[len(refs) * 2 // 3 :]
    half = refs[0].shape[0]
    for k, out in enumerate(outs):
        out[:half, :] = refs[2 * k][...]
        out[half:, :] = refs[2 * k + 1][...]


def ring_gather(block, stage):
    half = block.shape[0] // 2
    before_top = plane_send(block[:half], 1, stage)
    after_bottom = plane_send(block[half:], -1, stage)
    before_bottom = plane_send(block[half:], 1, stage)
    after_top = plane_send(block[:half], -1, stage)
    far_top = plane_send(before_top, 1, stage)
    far_bottom = plane_send(after_bottom, -1, stage)
    whole = like(block.shape, block.dtype)
    after, before = call(join_kernel, [whole] * 2, [after_top, after_bottom, before_top, before_bottom])
    return [block, after, jnp.concatenate([far_top, far_bottom], axis=0), before]


def short_ring_gather(block, stage):
    before = plane_send(block, 1, stage)
    after = plane_send(block, -1, stage)
    far = plane_send(before, 1, stage)
    return [block, after, far, before]


def ring_sum(after, far, before, stage):
    half = far.shape[0] // 2
    top = plane_send(far[:half].astype(BF16), 1, stage)
    bottom = plane_send(far[half:].astype(BF16), -1, stage)
    out = like(after.shape, BF16)
    up, down = call(ring_add_kernel, [out] * 2, [after, before, top, bottom])
    return plane_send(up, 1, stage), plane_send(down, -1, stage)


def short_ring_sum(after, far, before, stage):
    from_far = plane_send(far, 2, stage)
    from_after = plane_send(before, -1, stage)
    from_before = plane_send(after, 1, stage)
    return from_before, from_after, from_far


def z_gather(block):
    rows = block.shape[0] // 2
    one = z_send(block, 1)
    two = z_send(one, 1)
    three = z_send(two, 1)
    four = z_send(three[:rows], 1)
    return (one, two), (three, block, four), (2 * rows, 2 * rows), (2 * rows, rows, rows)


def z_sum(parts):
    got = []
    for terms, first, count in reversed(parts):
        block = call(functools.partial(z_add_kernel, first), [like((count, terms.shape[1]), BF16)], [terms] + got)[0]
        got = [z_send(block, -1)]
    return got[0]


def body(later_tokens, earlier_tokens, earlier_cotangent, gate_weight, up_weight, down_weight, gate_sum, up_sum, down_sum):
    tokens, width = later_tokens.shape
    hidden = down_weight.shape[0]
    y, x, c = lax.axis_index("y"), lax.axis_index("x"), lax.axis_index("c")
    k = jnp.arange(16, dtype=jnp.int32)
    high, low = k // 4, k % 4
    order0 = (y + high) % NY * NX + (x + low) % NX
    order1 = (y + low) % NY * NX + (x + high) % NX
    place0 = (high - y) % NY * 4 + (low - x) % NX
    place1 = (low - x) % NX * 4 + (high - y) % NY
    order = jnp.where(c == 0, order0, order1)
    own_place = jnp.where(c == 0, place0, place1)
    other_place = jnp.where(c == 0, place1, place0)

    packed = jnp.concatenate([gate_weight.T, up_weight.T, down_weight], axis=0)
    line = jnp.concatenate(short_ring_gather(packed, 1), axis=1)
    line, after, far, before = ring_gather(line, 2)
    pieces = [line, after, before, far]
    others = [swap(p) for p in pieces]
    weights = call(assemble_kernel, [like((3, 2 * hidden, width), BF16)], pieces + others)

    own = jnp.concatenate([earlier_tokens, earlier_cotangent, later_tokens], axis=1)
    earlier_block, later_block = call(
        pack_tokens_kernel,
        [like((2 * tokens, 2 * width), BF16), like((2 * tokens, width), BF16)],
        [order, own, swap(own)],
        [SMEM] + [VMEM] * 2,
    )
    near, far, near_counts, far_counts = z_gather(earlier_block)
    later_near, later_far, _, _ = z_gather(later_block)
    rows = 4 * tokens
    units = 2 * hidden

    def earlier(pieces, counts):
        return call(
            functools.partial(grads_kernel, counts),
            [like((rows, 2 * width), BF16), like((3, rows, units), BF16)],
            list(pieces) + list(weights),
            flops=6 * rows * units * width,
            scratch=[pltpu.VMEM((3, rows, units), F32)],
            limit=6,
        )

    def later(pieces, counts):
        return call(
            functools.partial(later_kernel, counts),
            [like((rows, width), F32)],
            list(pieces) + list(weights),
            flops=6 * rows * units * width,
            scratch=[pltpu.VMEM((rows, width), BF16)]
            + [pltpu.VMEM((2, rows, units), F32), pltpu.VMEM((rows, units), BF16)],
            limit=6,
        )[0]

    x_a, grads_a = earlier(near, near_counts)
    x_b, grads_b = earlier(far, far_counts)
    terms = call(
        terms_kernel,
        [like((2 * rows, width), F32)],
        [grads_a, grads_b, *weights],
        flops=8 * rows * units * width,
        scratch=[pltpu.VMEM((2, 2 * rows, units), BF16)],
        limit=6,
    )[0]
    later_a = later(later_near, near_counts)
    later_b = later(later_far, far_counts)
    pair = 2 * tokens
    sums = [
        z_sum([(terms, pair, pair), (terms, 2 * pair, pair), (terms, 3 * pair + tokens, tokens)]),
        z_sum([(later_a, pair, pair), (later_b, 0, pair), (later_b, pair + tokens, tokens)]),
    ]
    both = call(last_add_kernel, [like((pair, 2 * width), BF16)], [terms, later_a] + sums)[0]
    mine = z_send(both, -1)
    other = swap(mine[tokens:])
    earlier_grad, later_output = call(
        unpack_kernel,
        [like((tokens, width), BF16)] * 2,
        [own_place, other_place, terms, later_b, mine, other],
        [SMEM] * 2 + [VMEM] * 4,
    )

    so_far = call(
        weight_grads_kernel,
        [like((3, hidden, width), F32), like((3, hidden, width), BF16)],
        [grads_a, x_a],
        flops=6 * rows * units * width,
        limit=6,
    )
    sent, held = call(
        more_weight_grads_kernel,
        [like((3 * hidden, width), BF16), like((3, hidden, width), F32)],
        [grads_b, x_b, *so_far],
        flops=6 * rows * units * width,
        limit=6,
    )
    sent = swap(sent)
    piece = like((3 * hidden, width // 4), F32)
    here, after, far, before = call(pair_sum_kernel, [piece] * 4, [held, sent])
    from_before, from_after = ring_sum(after, far, before, 2)
    strip = like((3 * hidden, LANES), F32)
    strip_sent = like((3 * hidden, LANES), BF16)
    here, after, far, before = call(
        line_sum_kernel, [strip, strip_sent, strip_sent, strip_sent], [here, from_before, from_after]
    )
    total = here
    for part in short_ring_sum(after, far, before, 1):
        total = total + part.astype(F32)
    gate_total = gate_sum + total[:hidden].T
    up_total = up_sum + total[hidden : 2 * hidden].T
    down_total = down_sum + total[2 * hidden :]
    return later_output, earlier_grad, gate_total, up_total, down_total


def solution(mesh):
    finer = Mesh(mesh.devices.reshape(NY, NX, NZ, 2), ("y", "x", "z", "c"))
    rows, cols = ("y", "x"), ("z", "c")
    token = P(rows + cols, None)
    in_specs = (token,) * 3 + (P(rows, cols), P(rows, cols), P(cols, rows)) * 2
    out_specs = (token, token, P(rows, cols), P(rows, cols), P(cols, rows))

    return jax.shard_map(body, mesh=finer, in_specs=in_specs, out_specs=out_specs, check_vma=False)
```

```python
import functools

import jax
import jax.numpy as jnp
from jax import lax
from jax.experimental import pallas as pl
from jax.experimental.pallas import tpu as pltpu
from jax.sharding import Mesh
from jax.sharding import PartitionSpec as P


NY, NX, NZ = 4, 4, 8
LANES = 128
TILE = 1024
STEP = 16
F32, BF16 = jnp.float32, jnp.bfloat16
VMEM = pl.BlockSpec(memory_space=pltpu.VMEM)
SMEM = pl.BlockSpec(memory_space=pltpu.SMEM)


def z_pairs(step):
    return [
        (z * 2 + c, (z + (step if c == 0 else -step)) % NZ * 2 + c)
        for z in range(NZ)
        for c in range(2)
    ]


def plane_pairs(step, stage):
    pairs = []
    for y in range(NY):
        for x in range(NX):
            for c in range(2):
                along_x = (stage == 1) == (c == 0)
                to_y = y if along_x else (y + step) % NY
                to_x = (x + step) % NX if along_x else x
                pairs.append(((y * NX + x) * 2 + c, (to_y * NX + to_x) * 2 + c))
    return pairs


def z_send(value, step):
    return lax.ppermute(value, ("z", "c"), z_pairs(step))


def plane_send(value, step, stage):
    return lax.ppermute(value, ("y", "x", "c"), plane_pairs(step, stage))


def swap(value):
    return lax.ppermute(value, "c", [(0, 1), (1, 0)])


def call(kernel, outs, ins, specs=None, flops=0, scratch=(), limit=4):
    moved = sum(o.size * o.dtype.itemsize for o in outs) + sum(i.size * i.dtype.itemsize for i in ins)
    return pl.pallas_call(
        kernel,
        out_shape=outs,
        in_specs=specs or [VMEM] * len(ins),
        out_specs=[VMEM] * len(outs),
        scratch_shapes=scratch,
        compiler_params=pltpu.CompilerParams(vmem_limit_bytes=int(limit * 2**20)),
        cost_estimate=pl.CostEstimate(flops=flops or moved, bytes_accessed=moved, transcendentals=0),
    )(*ins)


def like(shape, dtype):
    return jax.ShapeDtypeStruct(shape, dtype)


def lane(k):
    return pl.ds(k * LANES, LANES)


def pack_tokens_kernel(place_ref, own_ref, other_ref, earlier_ref, later_ref):
    rows, width = own_ref.shape[0], later_ref.shape[1]
    blocks = width // LANES
    for k in range(blocks):
        start = place_ref[k] * LANES
        for half, ref in enumerate((own_ref, other_ref)):
            to = slice(half * rows, (half + 1) * rows)
            for n, (out, first) in enumerate(((earlier_ref, 0), (earlier_ref, blocks), (later_ref, 0))):
                out[to, lane(first + k)] = ref[:, pl.ds(pl.multiple_of(n * width + start, LANES), LANES)]


def last_add_kernel(earlier_ref, later_ref, earlier_got, later_got, out_ref):
    rows, width = earlier_got.shape
    for n, (ref, got) in enumerate(((earlier_ref, earlier_got), (later_ref, later_got))):
        out_ref[:, n * width : (n + 1) * width] = (ref[:rows, :] + got[...].astype(F32)).astype(BF16)


def unpack_kernel(own_place_ref, other_place_ref, *refs):
    kept, mine_ref, other_ref, outs = refs[:2], refs[2], refs[3], refs[4:]
    width = kept[0].shape[1]
    rows = other_ref.shape[0]
    for k in range(width // LANES):
        own = pl.multiple_of(own_place_ref[k] * LANES, LANES)
        other = pl.multiple_of(other_place_ref[k] * LANES, LANES)
        for n in range(2):
            total = (
                kept[n][kept[n].shape[0] - 2 * rows : kept[n].shape[0] - rows, pl.ds(own, LANES)]
                + mine_ref[:rows, pl.ds(n * width + own, LANES)].astype(F32)
                + other_ref[:, pl.ds(n * width + other, LANES)].astype(F32)
            )
            outs[n][:, lane(k)] = total.astype(BF16)


def z_add_kernel(first, terms_ref, *refs):
    got, out = refs[0] if len(refs) > 1 else None, refs[-1]
    rows = out.shape[0]
    more = got.shape[0] if got is not None else 0
    if more:
        out[:more, :] = (terms_ref[first : first + more, :] + got[...].astype(F32)).astype(BF16)
    if more < rows:
        out[more:, :] = terms_ref[first + more : first + rows, :].astype(BF16)


def line_sum_kernel(here, from_before, from_after, *outs):
    rows = here.shape[0]

    @pl.loop(0, rows // STEP)
    def _(i):
        at = pl.ds(pl.multiple_of(i * STEP, STEP), STEP)
        for k, out in enumerate(outs):
            total = here[at, lane(k)] + from_before[at, lane(k)].astype(F32) + from_after[at, lane(k)].astype(F32)
            out[at, :] = total.astype(out.dtype)


def assemble_kernel(*refs):
    pieces, out = (refs[:4], refs[4:8]), refs[8]
    hidden = pieces[0][0].shape[0] // 3

    @pl.loop(0, hidden // STEP)
    def _(i):
        row = pl.multiple_of(i * STEP, STEP)
        for k in range(3):
            for n, b in enumerate((0, 1, 3, 2)):
                for core in range(2):
                    for a in range(4):
                        place = a * 4 + b if core else b * 4 + a
                        strip = pieces[core][n][pl.ds(k * hidden + row, STEP), lane(a)]
                        out[k, pl.ds(core * hidden + row, STEP), lane(place)] = strip


def pair_sum_kernel(*refs):
    own, other, outs = refs[0], refs[1], refs[2:]
    rows = own.shape[1]

    @pl.loop(0, rows // STEP)
    def _(i):
        row = pl.multiple_of(i * STEP, STEP)
        for b in range(4):
            for a in range(4):
                for k in range(3):
                    at = pl.ds(k * rows + row, STEP)
                    total = own[k, pl.ds(row, STEP), lane(b * 4 + a)] + other[at, lane(a * 4 + b)].astype(F32)
                    outs[b][at, lane(a)] = total


def ring_add_kernel(after, before, top, bottom, up, down):
    half = top.shape[0]

    @pl.loop(0, half // STEP)
    def _(i):
        at = pl.ds(pl.multiple_of(i * STEP, STEP), STEP)
        low = pl.ds(pl.multiple_of(half + i * STEP, STEP), STEP)
        up[at, :] = (after[at, :] + top[at, :].astype(F32)).astype(BF16)
        up[low, :] = after[low, :].astype(BF16)
        down[at, :] = before[at, :].astype(BF16)
        down[low, :] = (before[low, :] + bottom[at, :].astype(F32)).astype(BF16)


def nt_dot(left, right):
    return lax.dot_general(left, right, (((1,), (1,)), ((), ())), preferred_element_type=F32)


def tn_dot(left, right):
    return lax.dot_general(left, right, (((0,), (0,)), ((), ())), preferred_element_type=F32)


def gather_rows(pieces, x_ref):
    at = 0
    for ref, rows in pieces:
        x_ref[at : at + rows, :] = ref[:rows, :]
        at += rows


def grads_kernel(counts, *refs):
    pieces, refs = refs[: len(counts)], refs[len(counts) :]
    weights, x_ref, grads, made = refs
    gather_rows(list(zip(pieces, counts)), x_ref)
    width = weights.shape[2]

    @pl.loop(0, 3)
    def _(k):
        first = pl.multiple_of(k // 2 * width, width)
        made[k] = nt_dot(x_ref[:, pl.ds(first, width)], weights[k])

    @pl.loop(0, x_ref.shape[0] // STEP)
    def _(i):
        rows = pl.ds(pl.multiple_of(i * STEP, STEP), STEP)
        g, u, h = made[0, rows, :], made[1, rows, :], made[2, rows, :]
        s = jax.nn.sigmoid(g)
        a = g * s
        grads[0, rows, :] = (h * u * (s * (1.0 + g * (1.0 - s)))).astype(BF16)
        grads[1, rows, :] = (h * a).astype(BF16)
        grads[2, rows, :] = (a * u).astype(BF16)


def terms_kernel(grads, weights, terms):
    @pl.loop(0, terms.shape[1] // TILE)
    def _(n):
        at = pl.ds(pl.multiple_of(n * TILE, TILE), TILE)
        terms[:, at] = jnp.dot(grads[0], weights[0, :, at], preferred_element_type=F32) + jnp.dot(
            grads[1], weights[1, :, at], preferred_element_type=F32
        )


def later_kernel(counts, *refs):
    pieces, refs = refs[: len(counts)], refs[len(counts) :]
    weights, terms, x_ref, made, act = refs
    gather_rows(list(zip(pieces, counts)), x_ref)

    @pl.loop(0, 2)
    def _(k):
        made[k] = nt_dot(x_ref[...], weights[k])

    @pl.loop(0, x_ref.shape[0] // STEP)
    def _(i):
        rows = pl.ds(pl.multiple_of(i * STEP, STEP), STEP)
        g = made[0, rows, :]
        act[rows, :] = (g * jax.nn.sigmoid(g) * made[1, rows, :]).astype(BF16)

    @pl.loop(0, terms.shape[1] // TILE)
    def _(n):
        at = pl.ds(pl.multiple_of(n * TILE, TILE), TILE)
        terms[:, at] = jnp.dot(act[...], weights[2, :, at], preferred_element_type=F32)


def weight_grads_kernel(grads, x_ref, here, there):
    rows, width = here.shape[1:]

    @pl.loop(0, 3)
    def _(k):
        @pl.loop(0, width // TILE)
        def _(n):
            to = pl.ds(pl.multiple_of(n * TILE, TILE), TILE)
            at = pl.ds(pl.multiple_of(k // 2 * width + n * TILE, TILE), TILE)
            total = tn_dot(grads[k], x_ref[:, at])
            here[k, :, to] = total[:rows]
            there[k, :, to] = total[rows:].astype(BF16)


def more_weight_grads_kernel(grads, x_ref, here, there, sent, held):
    rows, width = held.shape[1:]

    @pl.loop(0, 3)
    def _(k):
        @pl.loop(0, width // TILE)
        def _(n):
            to = pl.ds(pl.multiple_of(n * TILE, TILE), TILE)
            at = pl.ds(pl.multiple_of(k // 2 * width + n * TILE, TILE), TILE)
            total = tn_dot(grads[k], x_ref[:, at])
            held[k, :, to] = here[k, :, to] + total[:rows]
            sent[pl.ds(pl.multiple_of(k * rows, STEP), rows), to] = (there[k, :, to].astype(F32) + total[rows:]).astype(BF16)


def join_kernel(*refs):
    outs = refs[len(refs) * 2 // 3 :]
    half = refs[0].shape[0]
    for k, out in enumerate(outs):
        out[:half, :] = refs[2 * k][...]
        out[half:, :] = refs[2 * k + 1][...]


def ring_gather(block, stage):
    half = block.shape[0] // 2
    before_top = plane_send(block[:half], 1, stage)
    after_bottom = plane_send(block[half:], -1, stage)
    before_bottom = plane_send(block[half:], 1, stage)
    after_top = plane_send(block[:half], -1, stage)
    far_top = plane_send(before_top, 1, stage)
    far_bottom = plane_send(after_bottom, -1, stage)
    whole = like(block.shape, block.dtype)
    after, before = call(join_kernel, [whole] * 2, [after_top, after_bottom, before_top, before_bottom])
    return [block, after, jnp.concatenate([far_top, far_bottom], axis=0), before]


def short_ring_gather(block, stage):
    before = plane_send(block, 1, stage)
    after = plane_send(block, -1, stage)
    far = plane_send(before, 1, stage)
    return [block, after, far, before]


def ring_sum(after, far, before, stage):
    half = far.shape[0] // 2
    top = plane_send(far[:half].astype(BF16), 1, stage)
    bottom = plane_send(far[half:].astype(BF16), -1, stage)
    out = like(after.shape, BF16)
    up, down = call(ring_add_kernel, [out] * 2, [after, before, top, bottom])
    return plane_send(up, 1, stage), plane_send(down, -1, stage)


def short_ring_sum(after, far, before, stage):
    from_far = plane_send(far, 2, stage)
    from_after = plane_send(before, -1, stage)
    from_before = plane_send(after, 1, stage)
    return from_before, from_after, from_far


def z_gather(block):
    rows = block.shape[0] // 2
    one = z_send(block, 1)
    two = z_send(one, 1)
    three = z_send(two, 1)
    four = z_send(three[:rows], 1)
    return (one, two), (three, block, four), (2 * rows, 2 * rows), (2 * rows, rows, rows)


def z_sum(parts):
    got = []
    for terms, first, count in reversed(parts):
        block = call(functools.partial(z_add_kernel, first), [like((count, terms.shape[1]), BF16)], [terms] + got)[0]
        got = [z_send(block, -1)]
    return got[0]


def body(later_tokens, earlier_tokens, earlier_cotangent, gate_weight, up_weight, down_weight, gate_sum, up_sum, down_sum):
    tokens, width = later_tokens.shape
    hidden = down_weight.shape[0]
    y, x, c = lax.axis_index("y"), lax.axis_index("x"), lax.axis_index("c")
    k = jnp.arange(16, dtype=jnp.int32)
    high, low = k // 4, k % 4
    order0 = (y + high) % NY * NX + (x + low) % NX
    order1 = (y + low) % NY * NX + (x + high) % NX
    place0 = (high - y) % NY * 4 + (low - x) % NX
    place1 = (low - x) % NX * 4 + (high - y) % NY
    order = jnp.where(c == 0, order0, order1)
    own_place = jnp.where(c == 0, place0, place1)
    other_place = jnp.where(c == 0, place1, place0)

    packed = jnp.concatenate([gate_weight.T, up_weight.T, down_weight], axis=0)
    line = jnp.concatenate(short_ring_gather(packed, 1), axis=1)
    line, after, far, before = ring_gather(line, 2)
    pieces = [line, after, before, far]
    others = [swap(p) for p in pieces]
    weights = call(assemble_kernel, [like((3, 2 * hidden, width), BF16)], pieces + others)

    own = jnp.concatenate([earlier_tokens, earlier_cotangent, later_tokens], axis=1)
    earlier_block, later_block = call(
        pack_tokens_kernel,
        [like((2 * tokens, 2 * width), BF16), like((2 * tokens, width), BF16)],
        [order, own, swap(own)],
        [SMEM] + [VMEM] * 2,
    )
    near, far, near_counts, far_counts = z_gather(earlier_block)
    later_near, later_far, _, _ = z_gather(later_block)
    rows = 4 * tokens
    units = 2 * hidden

    def earlier(pieces, counts):
        return call(
            functools.partial(grads_kernel, counts),
            [like((rows, 2 * width), BF16), like((3, rows, units), BF16)],
            list(pieces) + list(weights),
            flops=6 * rows * units * width,
            scratch=[pltpu.VMEM((3, rows, units), F32)],
            limit=6,
        )

    def later(pieces, counts):
        return call(
            functools.partial(later_kernel, counts),
            [like((rows, width), F32)],
            list(pieces) + list(weights),
            flops=6 * rows * units * width,
            scratch=[pltpu.VMEM((rows, width), BF16)]
            + [pltpu.VMEM((2, rows, units), F32), pltpu.VMEM((rows, units), BF16)],
            limit=6,
        )[0]

    x_a, grads_a = earlier(near, near_counts)
    x_b, grads_b = earlier(far, far_counts)
    terms_a, terms_b = (
        call(terms_kernel, [like((rows, width), F32)], [grads, *weights], flops=4 * rows * units * width, limit=8)[0]
        for grads in (grads_a, grads_b)
    )
    later_a = later(later_near, near_counts)
    later_b = later(later_far, far_counts)
    pair = 2 * tokens
    sums = [
        z_sum([(terms_a, pair, pair), (terms_b, 0, pair), (terms_b, pair + tokens, tokens)]),
        z_sum([(later_a, pair, pair), (later_b, 0, pair), (later_b, pair + tokens, tokens)]),
    ]
    both = call(last_add_kernel, [like((pair, 2 * width), BF16)], [terms_a, later_a] + sums)[0]
    mine = z_send(both, -1)
    other = swap(mine[tokens:])
    earlier_grad, later_output = call(
        unpack_kernel,
        [like((tokens, width), BF16)] * 2,
        [own_place, other_place, terms_b, later_b, mine, other],
        [SMEM] * 2 + [VMEM] * 4,
    )

    so_far = call(
        weight_grads_kernel,
        [like((3, hidden, width), F32), like((3, hidden, width), BF16)],
        [grads_a, x_a],
        flops=6 * rows * units * width,
        limit=6,
    )
    sent, held = call(
        more_weight_grads_kernel,
        [like((3 * hidden, width), BF16), like((3, hidden, width), F32)],
        [grads_b, x_b, *so_far],
        flops=6 * rows * units * width,
        limit=6,
    )
    sent = swap(sent)
    piece = like((3 * hidden, width // 4), F32)
    here, after, far, before = call(pair_sum_kernel, [piece] * 4, [held, sent])
    from_before, from_after = ring_sum(after, far, before, 2)
    strip = like((3 * hidden, LANES), F32)
    strip_sent = like((3 * hidden, LANES), BF16)
    here, after, far, before = call(
        line_sum_kernel, [strip, strip_sent, strip_sent, strip_sent], [here, from_before, from_after]
    )
    total = here
    for part in short_ring_sum(after, far, before, 1):
        total = total + part.astype(F32)
    gate_total = gate_sum + total[:hidden].T
    up_total = up_sum + total[hidden : 2 * hidden].T
    down_total = down_sum + total[2 * hidden :]
    return later_output, earlier_grad, gate_total, up_total, down_total


def solution(mesh):
    finer = Mesh(mesh.devices.reshape(NY, NX, NZ, 2), ("y", "x", "z", "c"))
    rows, cols = ("y", "x"), ("z", "c")
    token = P(rows + cols, None)
    in_specs = (token,) * 3 + (P(rows, cols), P(rows, cols), P(cols, rows)) * 2
    out_specs = (token, token, P(rows, cols), P(rows, cols), P(cols, rows))

    return jax.shard_map(body, mesh=finer, in_specs=in_specs, out_specs=out_specs, check_vma=False)
```
